32 devices in a mesh: ep: 8 (over z, y), tp: 4 (over x, core).
Axes of the slice: x: 2, y: 2, z: 4, core: 2. Of those that a mesh axis runs over, the one named last changes fastest.
Arguments:
- queries: bfloat16 [4096, 2048], P('ep', 'tp'), may hold values from -6 to 6
- key_rows: bfloat16 [4096, 2048], P('ep', 'tp'), may hold values from -6 to 6
- value_rows: bfloat16 [4096, 4096], P('ep', 'tp'), may hold values from -6 to 6
- gate_rows: bfloat16 [4096, 4096], P('ep', 'tp'), may hold values from -6 to 6
- log_decay: float32 [16, 4096], P('tp', 'ep'), may hold values from -1 to 0
- head_gain: float32 [4096], P('tp'), may hold values from 0.1 to 1.9
- out_weight: bfloat16 [4096, 4096], P('tp'), may hold values from -0.09375 to 0.09375
- expert_input: bfloat16 [4096, 4096], P('ep'), may hold values from -6 to 6
- input_gain: float32 [4096], replicated, may hold values from 0.1 to 1.9
- route_ids: int32 [4096, 2], P('ep'), may hold values from 0 to 7, as said below
- route_weight: float32 [4096, 2], P('ep'), may hold values from 0.1 to 0.9
- expert_gate: bfloat16 [8, 4096, 1024], P('ep', None, 'tp'), may hold values from -0.09375 to 0.09375
- expert_up: bfloat16 [8, 4096, 1024], P('ep', None, 'tp'), may hold values from -0.09375 to 0.09375
- expert_down: bfloat16 [8, 1024, 4096], P('ep', 'tp'), may hold values from -0.1875 to 0.1875
Outputs:
- mixer_out: bfloat16 [4096, 4096], P(('ep', 'tp'))
- expert_out: bfloat16 [4096, 4096], P('ep', 'tp')
The draws below stay inside these ranges and needn't reach their ends.
Inputs may be any that keep to these rules, and one draw needn't show every extreme that they name: `route_ids`: each row names two different experts of one group of 8 consecutive experts. On the rows of one device each group is named by exactly 512 rows, experts 2 i and 2 i + 1 together are named exactly 4 * 192 / 3 times, and no expert is named by more than 192 rows; one expert is named by exactly 192 rows of every device.
All inputs are finite; a program needn't handle non-finite values.
Results may differ from the reference program's by a relative error of at most 0.019.
Values may be sent and summed in bfloat16 or wider, within the bound.
A program may use at most 192 MiB of HBM per device.

```python
import math
import jax
import jax.numpy as jnp
from jax import lax

D = 4096
HEADS = 16
DK = 128
DV = 256
FF = 1024
EPG = 8
BLOCK = 512
TOK_A = 512
TOK_B = 512
EXPERTS = 8
GROUPS = 1
CAP = 192
FIRST_TOKENS = 4096
TOKENS_B = 4096
N_EP = 8
N_TP = 4


def draw_log_decay(key, part):
    random_subkeys = jax.random.split(jax.random.fold_in(key, 11), 7)
    quick = jax.random.uniform(random_subkeys[0], (HEADS,), jnp.float32) < 0.5
    quick_rate = 1.0 / jax.random.uniform(random_subkeys[1], (HEADS,), jnp.float32, 30.0, 50.0)
    steady_rate = 0.2 / FIRST_TOKENS * jnp.exp(jax.random.uniform(random_subkeys[2], (HEADS,), jnp.float32, -0.7, 0.0))
    head_rate = jnp.where(quick, quick_rate, steady_rate)
    shards = FIRST_TOKENS // TOK_A
    shard_factor = jnp.exp(jax.random.uniform(random_subkeys[3], (shards,), jnp.float32, 0.0, math.log(3.0)))
    position_factor = jnp.repeat(shard_factor, TOK_A, total_repeat_length=FIRST_TOKENS)
    roughness = jnp.exp(jax.random.uniform(random_subkeys[4], (HEADS, FIRST_TOKENS), jnp.float32, -0.35, 0.35))
    reference_level = -head_rate[:, None] * position_factor[None, :] * roughness
    spike_locations = jax.random.randint(random_subkeys[5], (2,), 0, FIRST_TOKENS)
    spike_removal = jnp.log(jax.random.uniform(random_subkeys[6], (2,), jnp.float32, 0.5, 0.8))
    spike_struck = (jnp.arange(FIRST_TOKENS)[None, :] == spike_locations[:, None]).astype(jnp.float32)
    spike_events = jnp.sum(spike_struck * spike_removal[:, None], axis=0)
    return reference_level + spike_events[None, :]


def route_block(block_key, busiest):
    random_subkeys = jax.random.split(block_key, 4)
    pair_count = EXPERTS // 2
    third = CAP // 3
    lifted = jax.random.randint(random_subkeys[0], (pair_count,), 0, 2 * third + 1)
    pair_index = jnp.arange(pair_count)
    lifted = jnp.where(pair_index == busiest // 2, 0, lifted)
    upper_side = jax.random.randint(random_subkeys[1], (pair_count,), 0, 2)
    upper_side = jnp.where(pair_index == busiest // 2, busiest % 2, upper_side)
    heavy = CAP - lifted
    lighter = third + lifted
    even_load = jnp.where(upper_side == 0, heavy, lighter)
    odd_load = jnp.where(upper_side == 0, lighter, heavy)
    loads = jnp.stack([even_load, odd_load], axis=1).reshape(GROUPS, EPG)
    run_ends = jnp.cumsum(loads, axis=1)
    group_rows = TOK_B // GROUPS
    tickets = jnp.arange(2 * group_rows)
    local_expert = jnp.sum((tickets[None, :, None] >= run_ends[:, None, :]).astype(jnp.int32), axis=2)
    shuffled = jax.random.permutation(random_subkeys[2], TOK_B)
    group_of = shuffled // group_rows
    place_of = shuffled % group_rows
    first_pick = group_of * EPG + local_expert[group_of, place_of]
    second_pick = group_of * EPG + local_expert[group_of, place_of + group_rows]
    swapped = jax.random.randint(random_subkeys[3], (TOK_B,), 0, 2)
    column_one = jnp.where(swapped == 0, first_pick, second_pick)
    column_two = jnp.where(swapped == 0, second_pick, first_pick)
    return jnp.stack([column_one, column_two], axis=1).astype(jnp.int32)


def draw_route_ids(key, part):
    busiest = jax.random.randint(jax.random.fold_in(key, 7), (), 0, EXPERTS)
    shards = TOKENS_B // TOK_B
    stacked = jax.vmap(lambda shard_index: route_block(jax.random.fold_in(key, shard_index + 100), busiest))(jnp.arange(shards))
    return stacked.reshape(TOKENS_B, 2)


def level_of(rng, extent, cuts, smallest, largest):
    loudness, own = 1.0, jax.random.fold_in(rng, 6)
    for position, parts in cuts:
        steps = jnp.exp(jax.random.uniform(jax.random.fold_in(own, position), (parts,), jnp.float32, smallest / len(cuts), largest / len(cuts)))
        loudness = loudness * jnp.repeat(steps, extent[position] // parts).reshape([-1 if axis == position else 1 for axis in range(len(extent))])
    return loudness


def normal_values(rng, extent, scale, limit, cuts=(), kind=jnp.bfloat16):
    level = level_of(rng, extent, cuts, -0.22, 0.18) if cuts else 1.0
    entries = jax.random.normal(rng, extent, jnp.float32) * scale * level
    return jnp.minimum(jnp.maximum(entries, -limit), limit).astype(kind)


def setup_inputs(seed: int = 0) -> dict:
    keys = jax.random.split(jax.random.key(seed), 15)
    queries = normal_values(keys[0], (FIRST_TOKENS, HEADS * DK), 1.0, 6.0, ((0, 8), (1, 4)))
    key_rows = normal_values(keys[1], (FIRST_TOKENS, HEADS * DK), 1.0, 6.0, ((0, 8), (1, 4)))
    value_rows = normal_values(keys[2], (FIRST_TOKENS, HEADS * DV), 1.0, 6.0, ((0, 8), (1, 4)))
    gate_rows = normal_values(keys[3], (FIRST_TOKENS, HEADS * DV), 1.0, 6.0, ((0, 8), (1, 4)))
    log_decay = draw_log_decay(jax.random.fold_in(keys[14], 71), 0)
    head_gain = jnp.clip(1.0 + 0.18 * jax.random.normal(keys[5], (HEADS * DV,), jnp.float32), 0.1, 1.9)
    out_weight = normal_values(keys[6], (HEADS * DV, D), (HEADS * DV) ** -0.5, 0.09375, ((0, 4),))
    expert_input = normal_values(keys[7], (TOKENS_B, D), 1.0, 6.0, ((0, 8),))
    input_gain = jnp.clip(1.0 + 0.18 * jax.random.normal(keys[8], (D,), jnp.float32), 0.1, 1.9)
    route_ids = draw_route_ids(jax.random.fold_in(keys[14], 71), 0)
    route_weight = jnp.clip(0.1 + 0.79999997 * jax.random.uniform(keys[10], (TOKENS_B, 2), jnp.float32) ** level_of(keys[10], (TOKENS_B, 2), ((0, 8),), -0.2, 0.2), 0.1, 0.9)
    expert_gate = normal_values(keys[11], (EXPERTS, D, FF), D ** -0.5, 0.09375, ((0, 8), (2, 4)))
    expert_up = normal_values(keys[12], (EXPERTS, D, FF), D ** -0.5, 0.09375, ((0, 8), (2, 4)))
    expert_down = normal_values(keys[13], (EXPERTS, FF, D), FF ** -0.5, 0.1875, ((0, 8), (1, 4)))
    return dict(queries=queries, key_rows=key_rows, value_rows=value_rows, gate_rows=gate_rows, log_decay=log_decay, head_gain=head_gain, out_weight=out_weight, expert_input=expert_input, input_gain=input_gain, route_ids=route_ids, route_weight=route_weight, expert_gate=expert_gate, expert_up=expert_up, expert_down=expert_down)


epsilon = 1e-06
theta_base = 10000.0
largest_entry = lax.Precision.HIGHEST

def rotate(values, positions):
    half_dim = values.shape[-1] // 2
    frequency = theta_base ** (-jnp.arange(half_dim, dtype=jnp.float32) / half_dim)
    angles = positions.astype(jnp.float32)[:, None, None] * frequency
    cosine = jnp.cos(angles)
    sine_wave = jnp.sin(angles)
    first_half = values[..., :half_dim]
    second = values[..., half_dim:]
    return jnp.concatenate([first_half * cosine - second * sine_wave, second * cosine + first_half * sine_wave], axis=-1)

def round_back(values):
    return lax.optimization_barrier(values.astype(jnp.bfloat16)).astype(jnp.float32)

def grouped_product(hidden, weight, groups):
    width = hidden.shape[1] // groups
    summed = jnp.zeros((hidden.shape[0], weight.shape[1]), jnp.float32)
    for group_index in range(groups):
        lower = group_index * width
        partial_sum = jnp.dot(hidden[:, lower:lower + width], weight[lower:lower + width], preferred_element_type=jnp.float32)
        summed = summed + round_back(partial_sum)
    return summed.astype(jnp.bfloat16)

def to_blocks(array, blocks):
    return array.reshape(blocks, array.shape[0] // blocks, array.shape[1], array.shape[2])

def retention(queries, key_rows, value_rows, gate_rows, log_decay, head_gain):
    tokens_all = queries.shape[0]
    positions = jnp.arange(tokens_all, dtype=jnp.int32)
    blocks = tokens_all // BLOCK
    query_rot = to_blocks(rotate(queries.astype(jnp.float32).reshape(tokens_all, HEADS, DK), positions), blocks)
    key_rot = to_blocks(rotate(key_rows.astype(jnp.float32).reshape(tokens_all, HEADS, DK), positions) * DK ** (-0.5), blocks)
    value_all = to_blocks(value_rows.astype(jnp.float32).reshape(tokens_all, HEADS, DV), blocks)
    running = jnp.cumsum(log_decay.reshape(HEADS, blocks, BLOCK), axis=2)
    causal = jnp.arange(BLOCK)[:, None] >= jnp.arange(BLOCK)[None, :]

    def advance(carried, inputs):
        query_tile, key_tile, value_blk, running_blk = inputs
        spread = running_blk[:, :, None] - running_blk[:, None, :]
        weight_table = jnp.exp(jnp.where(causal[None], spread, -jnp.inf))
        score_matrix = jnp.einsum('xya,zya->yxz', query_tile, key_tile, precision=largest_entry) * weight_table
        inside = jnp.einsum('hlm,mhe->lhe', score_matrix, value_blk, precision=largest_entry)
        outside = jnp.einsum('lhd,hl,hde->lhe', query_tile, jnp.exp(running_blk), carried, precision=largest_entry)
        ending = running_blk[:, -1]
        kept = jnp.exp(ending[:, None] - running_blk)
        updated = jnp.exp(ending)[:, None, None] * carried + jnp.einsum('lhd,hl,lhe->hde', key_tile, kept, value_blk, precision=largest_entry)
        return (updated, inside + outside)
    final_state, mixed = lax.scan(advance, jnp.zeros((HEADS, DK, DV), jnp.float32), (query_rot, key_rot, value_all, jnp.moveaxis(running, 1, 0)))
    mixed = mixed.reshape(tokens_all, HEADS, DV)
    centered = mixed - lax.optimization_barrier(jnp.mean(mixed, axis=-1, keepdims=True))
    normed = centered * lax.rsqrt(lax.optimization_barrier(jnp.mean(centered * centered, axis=-1, keepdims=True)) + epsilon) * head_gain.reshape(HEADS, DV)
    return (jax.nn.silu(gate_rows.astype(jnp.float32)) * normed.reshape(tokens_all, HEADS * DV)).astype(jnp.bfloat16)

def expert_layer(expert_input, input_gain, route_ids, route_weight, expert_gate, expert_up, expert_down):
    tokens_all = expert_input.shape[0]
    widened = expert_input.astype(jnp.float32)
    normed = (widened * lax.rsqrt(lax.optimization_barrier(jnp.mean(widened * widened, axis=-1, keepdims=True)) + epsilon) * input_gain).astype(jnp.bfloat16)
    padded = jnp.concatenate([normed, jnp.zeros((1, D), jnp.bfloat16)], axis=0)
    slots = N_EP * CAP
    flat_ids = route_ids.reshape(-1).astype(jnp.int32)
    matches = (flat_ids[:, None] == jnp.arange(EXPERTS, dtype=jnp.int32)[None, :]).astype(jnp.int32)
    slot_rank = lax.optimization_barrier(jnp.sum((jnp.cumsum(matches, axis=0) - matches) * matches, axis=1)).astype(jnp.int32)
    target = (flat_ids * slots + slot_rank).astype(jnp.int32)
    owners = (jnp.arange(2 * tokens_all, dtype=jnp.int32) // 2).astype(jnp.int32)
    slot_table = jnp.full((EXPERTS * slots,), tokens_all, jnp.int32).at[target].set(owners)

    def one_expert(inputs):
        row_index, gate_matrix, up_matrix, down_matrix = inputs
        chosen = padded[row_index]
        gate_val = jnp.dot(chosen, gate_matrix, preferred_element_type=jnp.float32)
        up_val = jnp.dot(chosen, up_matrix, preferred_element_type=jnp.float32)
        inner_rows = (jax.nn.silu(gate_val) * up_val).astype(jnp.bfloat16)
        return grouped_product(inner_rows, down_matrix, N_TP)
    results = lax.map(one_expert, (slot_table.reshape(EXPERTS, slots), expert_gate, expert_up, expert_down))
    picked = results.reshape(EXPERTS * slots, D)[target].reshape(tokens_all, 2, D).astype(jnp.float32)
    return lax.optimization_barrier(jnp.sum(picked * route_weight[:, :, None], axis=1)).astype(jnp.bfloat16)

def reference(queries, key_rows, value_rows, gate_rows, log_decay, head_gain, out_weight, expert_input, input_gain, route_ids, route_weight, expert_gate, expert_up, expert_down):
    hidden = retention(queries, key_rows, value_rows, gate_rows, log_decay, head_gain)
    mixer_out = grouped_product(hidden, out_weight, N_TP)
    expert_out = expert_layer(expert_input, input_gain, route_ids, route_weight, expert_gate, expert_up, expert_down)
    return (mixer_out, expert_out)
```

```python
import functools
import math

import jax
import jax.numpy as jnp
from jax import lax
from jax.experimental import pallas as pl
from jax.experimental.pallas import tpu as pltpu
from jax.sharding import PartitionSpec as P

MESH = pl.DeviceIdType.MESH
F32, BF16 = jnp.float32, jnp.bfloat16
epsilon = 1e-06
theta_base = 10000.0
TAIL = 16
LAG = 4


def xor(a, b, bits):
    total = 0
    for bit in range(bits):
        step = 1 << bit
        total = total + step * (((a // step) + (b // step)) % 2)
    return total


def dot(a, b, dims=((1,), (0,))):
    return lax.dot_general(a, b, (dims, ((), ())), preferred_element_type=F32)


def kernel(
    sizes,
    outgoing, gate, up, down, combine,
    queries, keys, values, gates, cosine, sine, run_col, run_row, gain, out_weight,
    mixer_out, expert_out,
    tok, gu, dn, wt, inn, res, ret,
    q_in, k_in, v_in, g_in, cos_s, sin_s, rc_s, rr_s, gain_s, ow,
    qhi, qlo, khi, klo, state, carry, packed, mixed, hidden, part, from_sib, from_far,
    acc,
    load_sem, ow_sem,
    disp_s, disp_r, tok_s, tok_r, inn_s, inn_r, ret_s, ret_r, dn_s, dn_r,
    chain_s, chain_r, mix_s, mix_r,
):
    n_ep, n_tp, heads, dk, dv = sizes
    bits = int(math.log2(n_ep))
    ep = lax.axis_index("ep")
    tp = lax.axis_index("tp")
    sib = xor(tp, 1, 2)
    far = xor(tp, 2, 2)
    diag = xor(tp, 3, 2)
    length = queries.shape[0]
    share, width = tok.shape[2], tok.shape[3]
    rows = n_tp * share
    units = gate.shape[2]
    cols = width // n_tp
    wide = ow.shape[2]
    n_wide = width // wide

    def local(k, src, dst):
        return pltpu.make_async_copy(src, dst, load_sem.at[k])

    def remote(src, dst, send, recv, device):
        return pltpu.make_async_remote_copy(
            src_ref=src, dst_ref=dst, send_sem=send, recv_sem=recv,
            device_id=device, device_id_type=MESH,
        )

    def dispatch(m):
        peer = xor(ep, m, bits)
        return remote(outgoing.at[peer], tok.at[ep, tp], disp_s.at[m], disp_r.at[m], (peer, tp))

    def dispatch_in(m):
        peer = xor(ep, m, bits)
        return remote(outgoing.at[peer], tok.at[peer, tp], disp_s.at[m], disp_r.at[m], (peer, tp))

    def own_rows():
        return pltpu.make_async_copy(outgoing.at[ep], tok.at[ep, tp], disp_r.at[0])

    def trade(ref, s, m, kind, send, recv, incoming=False):
        if incoming:
            piece = (far, sib, diag)[kind]
        else:
            piece = (tp, tp, far)[kind]
        device = (ep, (far, sib, sib)[kind])
        return remote(ref.at[s, piece], ref.at[s, piece], send.at[m, kind], recv.at[m, kind], device)

    def give_back(m):
        peer = xor(ep, m, bits)
        return remote(res.at[peer], ret.at[ep], ret_s.at[m], ret_r.at[m], (peer, tp))

    def give_back_in(m):
        peer = xor(ep, m, bits)
        return remote(res.at[peer], ret.at[peer], ret_s.at[m], ret_r.at[m], (peer, tp))

    def dn_out(j):
        peer = xor(tp, j, 2)
        start = pl.multiple_of(peer * cols, cols)
        return remote(down.at[0, :, pl.ds(start, cols)], dn.at[tp], dn_s.at[j], dn_r.at[j], (ep, peer))

    def dn_in(j):
        peer = xor(tp, j, 2)
        start = pl.multiple_of(peer * cols, cols)
        return remote(down.at[0, :, pl.ds(start, cols)], dn.at[peer], dn_s.at[j], dn_r.at[j], (ep, peer))

    def dn_own():
        start = pl.multiple_of(tp * cols, cols)
        return pltpu.make_async_copy(down.at[0, :, pl.ds(start, cols)], dn.at[tp], dn_r.at[0])

    def chain_out():
        return remote(packed, carry, chain_s, chain_r, (ep + 1, tp))

    def chain_in():
        return remote(packed, carry, chain_s, chain_r, (ep - 1, tp))

    def ow_copy(j, slot):
        start = pl.multiple_of(j * wide, wide)
        return pltpu.make_async_copy(out_weight.at[:, pl.ds(start, wide)], ow.at[slot], ow_sem.at[slot])

    def mix_copy(kind, incoming=False):
        if kind == 0:
            return remote(part.at[sib], from_sib.at[0], mix_s.at[0], mix_r.at[0], (ep, sib))
        if kind == 1:
            return remote(part.at[diag], from_sib.at[1], mix_s.at[1], mix_r.at[1], (ep, sib))
        return remote(part.at[far], from_far, mix_s.at[2], mix_r.at[2], (ep, far))

    loads = [
        local(0, queries, q_in), local(1, keys, k_in), local(2, values, v_in),
        local(3, gates, g_in), local(4, cosine, cos_s), local(5, sine, sin_s),
        local(6, run_col, rc_s), local(7, run_row, rr_s), local(8, gain, gain_s),
        local(9, gate.at[0], gu.at[:, pl.ds(0, units)]),
        local(10, up.at[0], gu.at[:, pl.ds(units, units)]),
        local(11, combine, wt),
    ]

    barrier = pltpu.get_barrier_semaphore()

    @pl.loop(1, n_ep)
    def _(m):
        pl.semaphore_signal(barrier, inc=1, device_id=(xor(ep, m, bits), tp), device_id_type=MESH)

    @pl.loop(1, n_tp)
    def _(j):
        pl.semaphore_signal(barrier, inc=1, device_id=(ep, xor(tp, j, 2)), device_id_type=MESH)

    for k in (0, 1, 2, 4, 5, 6, 7):
        loads[k].start()
    dn_own().start()
    own_rows().start()
    for k in (9, 10, 3, 8, 11):
        loads[k].start()
    for j in range(2):
        ow_copy(j, j).start()
    pl.semaphore_wait(barrier, n_ep - 1 + n_tp - 1)

    @pl.loop(0, n_ep - 1)
    def _(i):
        dispatch(n_ep - 1 - i).start()

    for j in range(1, n_tp):
        dn_out(j).start()

    def begin_retention():
        for k in (0, 1, 2, 4, 5, 6, 7):
            loads[k].wait()

        def turn(x):
            return x * cos_s[...] + pltpu.roll(x, dk // 2, 1) * sin_s[...]

        scale = dk ** -0.5
        for h in range(heads):
            lanes = slice(h * dk, (h + 1) * dk)
            q = turn(q_in[:, lanes].astype(F32))
            high = q.astype(BF16)
            qhi[h] = high
            qlo[h] = (q - high.astype(F32)).astype(BF16)
            k = turn(k_in[:, lanes].astype(F32)) * scale
            high = k.astype(BF16)
            khi[h] = high
            klo[h] = (k - high.astype(F32)).astype(BF16)
            col = rc_s[h]
            ending = col[length - 1 : length]
            kept = (k * jnp.exp(ending - col)).astype(BF16)
            state[h] = dot(kept, v_in[:, h * dv : (h + 1) * dv], ((0,), (0,)))

    def send_state():
        for h in range(heads):
            packed[h] = state[h].astype(BF16)
        chain_out().start()

    def pass_state():
        for h in range(heads):
            ending = rc_s[h][length - 1 : length]
            packed[h] = (jnp.exp(ending) * carry[h].astype(F32) + state[h]).astype(BF16)
        chain_out().start()

    def inside(h):
        vh = v_in[:, pl.ds(pl.multiple_of(h * dv, dv), dv)]
        col = rc_s[h]
        row = rr_s[h]
        step = min(length, 128)
        for r in range(length // step):
            lines = slice(r * step, (r + 1) * step)
            seen = (r + 1) * step
            nt = ((1,), (1,))
            score = (
                dot(qhi[h, lines], khi[h, :seen], nt)
                + dot(qhi[h, lines], klo[h, :seen], nt)
                + dot(qlo[h, lines], khi[h, :seen], nt)
            )
            later = lax.broadcasted_iota(jnp.int32, (step, seen), 0) + r * step
            earlier = lax.broadcasted_iota(jnp.int32, (step, seen), 1)
            spread = col[lines] - row[:, :seen]
            weight = jnp.exp(jnp.where(later >= earlier, spread, -jnp.inf))
            mixed[h, lines] = dot((score * weight).astype(BF16), vh[:seen])

    def finish_retention():
        loads[3].wait()
        loads[8].wait()
        step = min(length, 128)
        chunks = length // step

        @pl.loop(0, heads * chunks)
        def _(c):
            h = c // chunks
            lines = pl.ds(pl.multiple_of((c % chunks) * step, step), step)
            lanes = pl.ds(pl.multiple_of(h * dv, dv), dv)
            begun = carry[h]
            outside = dot(qhi[h, lines], begun) + dot(qlo[h, lines], begun)
            o = mixed[h, lines] + outside * jnp.exp(rc_s[h, lines])
            centered = o - jnp.mean(o, axis=1, keepdims=True)
            normed = (
                centered
                * lax.rsqrt(jnp.mean(centered * centered, axis=1, keepdims=True) + epsilon)
                * gain_s[:, lanes]
            )
            g = g_in[lines, lanes].astype(F32)
            hidden[lines, lanes] = (g / (1.0 + jnp.exp(-g)) * normed).astype(BF16)

        @pl.loop(0, n_wide)
        def _(j):
            slot = j % 2
            ow_copy(j, slot).wait()
            total = dot(hidden[...], ow[slot]).astype(BF16)
            here = pl.ds(pl.multiple_of(j * wide, wide), wide)
            part[:, :, here] = total.reshape(n_tp, length // n_tp, wide)

            @pl.when(j + 2 < n_wide)
            def _():
                ow_copy(j + 2, slot).start()

        mix_copy(1).start()
        mix_copy(0).start()

    def forward_mix():
        mix_copy(1).wait_send()
        mix_copy(1).wait_recv()
        part[far] = (part[far].astype(F32) + from_sib[1].astype(F32)).astype(BF16)
        mix_copy(2).start()

    @pl.loop(0, n_ep + LAG)
    def _(i):
        @pl.when(i < n_ep)
        def _():
            m = n_ep - 1 - i
            s = xor(ep, m, bits)

            @pl.when(m > 0)
            def _():
                dispatch_in(m).wait_recv()

            @pl.when(m == 0)
            def _():
                own_rows().wait()

            trade(tok, s, m, 0, tok_s, tok_r).start()
            trade(tok, s, m, 1, tok_s, tok_r).start()

        @pl.when((i >= 1) & (i < n_ep + 1))
        def _():
            m = n_ep - i
            s = xor(ep, m, bits)
            trade(tok, s, m, 0, tok_s, tok_r, True).wait_recv()
            trade(tok, s, m, 2, tok_s, tok_r).start()

        @pl.when(i == 0)
        def _():
            begin_retention()

            @pl.when(ep == 0)
            def _():
                carry[...] = jnp.zeros_like(carry)
                send_state()

        @pl.when((i == ep) & (ep > 0))
        def _():
            chain_in().wait_recv()

            @pl.when(ep < n_ep - 1)
            def _():
                pass_state()

        @pl.when((i >= 1) & (i < 1 + heads))
        def _():
            inside(i - 1)

        @pl.when(i == 1)
        def _():
            loads[9].wait()
            loads[10].wait()

        @pl.when((i >= 2) & (i < n_ep + 2))
        def _():
            m = n_ep + 1 - i
            s = xor(ep, m, bits)
            trade(tok, s, m, 1, tok_s, tok_r, True).wait_recv()
            trade(tok, s, m, 2, tok_s, tok_r, True).wait_recv()
            both = dot(tok[s].reshape(rows, width), gu[...])
            g = both[:, :units]
            inn[s, tp] = (g / (1.0 + jnp.exp(-g)) * both[:, units:]).astype(BF16)
            trade(inn, s, m, 0, inn_s, inn_r).start()
            trade(inn, s, m, 1, inn_s, inn_r).start()

        @pl.when((i >= 3) & (i < n_ep + 3))
        def _():
            m = n_ep + 2 - i
            s = xor(ep, m, bits)
            trade(inn, s, m, 0, inn_s, inn_r, True).wait_recv()
            trade(inn, s, m, 2, inn_s, inn_r).start()

        @pl.when(i == 3)
        def _():
            dn_own().wait()
            for j in range(1, n_tp):
                dn_in(j).wait_recv()

        @pl.when(i >= 4)
        def _():
            m = n_ep + 3 - i
            s = xor(ep, m, bits)
            trade(inn, s, m, 1, inn_s, inn_r, True).wait_recv()
            trade(inn, s, m, 2, inn_s, inn_r, True).wait_recv()
            total = dot(inn[s, 0], dn[0])
            for t in range(1, n_tp):
                total = total + dot(inn[s, t], dn[t])
            res[s] = total.astype(BF16)

            @pl.when(m > 0)
            def _():
                give_back(m).start()

        @pl.when(i == n_ep)
        def _():
            finish_retention()

        @pl.when(i == n_ep + 2)
        def _():
            forward_mix()

    loads[11].wait()
    acc[...] = dot(wt[ep], res[ep], ((0,), (0,)))

    @pl.loop(0, n_ep - 1)
    def _(i):
        m = n_ep - 1 - i
        s = xor(ep, m, bits)
        give_back_in(m).wait_recv()
        acc[...] += dot(wt[s], ret[s], ((0,), (0,)))

    expert_out[...] = acc[...].astype(BF16)

    mix_copy(0).wait_recv()
    mix_copy(2).wait_recv()
    mixer_out[...] = (
        part[tp].astype(F32) + from_sib[0].astype(F32) + from_far[...].astype(F32)
    ).astype(BF16)

    mix_copy(0).wait_send()
    mix_copy(2).wait_send()

    @pl.when(ep < n_ep - 1)
    def _():
        chain_out().wait_send()

    for j in range(1, n_tp):
        dn_out(j).wait_send()

    @pl.loop(0, n_ep)
    def _(m):
        s = xor(ep, m, bits)
        for kind in range(3):
            trade(tok, s, m, kind, tok_s, tok_r).wait_send()
            trade(inn, s, m, kind, inn_s, inn_r).wait_send()

    @pl.loop(1, n_ep)
    def _(m):
        dispatch(m).wait_send()
        give_back(m).wait_send()


def body(
    queries, key_rows, value_rows, gate_rows, log_decay, head_gain, out_weight,
    expert_input, input_gain, route_ids, route_weight, expert_gate, expert_up, expert_down,
):
    n_tp = lax.axis_size("tp")
    n_ep = lax.axis_size("ep")
    tp_index = lax.axis_index("tp")
    width = out_weight.shape[1]
    tokens = expert_input.shape[0]
    n_experts = n_ep * expert_gate.shape[0]
    units = expert_gate.shape[2]
    capacity = 3 * tokens // n_experts
    share = -(-capacity // (n_tp * 16)) * 16
    rows = share * n_tp
    cols = width // n_tp
    length = queries.shape[0]
    heads = log_decay.shape[0]
    dk = queries.shape[1] // heads
    dv = value_rows.shape[1] // heads

    widened = expert_input.astype(F32)
    normed = (
        widened
        * lax.rsqrt(jnp.mean(widened * widened, axis=-1, keepdims=True) + epsilon)
        * input_gain
    ).astype(BF16)
    experts = jnp.arange(n_experts, dtype=jnp.int32)[None, :]
    named = [route_ids[:, k : k + 1] == experts for k in range(2)]
    both = (named[0] | named[1]).astype(BF16)
    order = jnp.arange(tokens, dtype=jnp.int32)
    earlier = (order[None, :] < order[:, None]).astype(BF16)
    ranks = jnp.dot(earlier, both, preferred_element_type=F32)
    code = [
        route_ids[:, k] * rows
        + jnp.sum(jnp.where(named[k], ranks, 0.0), axis=1).astype(jnp.int32)
        for k in range(2)
    ]
    slot = (
        experts[0][:, None] * rows
        + tp_index * share
        + jnp.arange(share, dtype=jnp.int32)[None, :]
    ).reshape(-1, 1)
    chosen = ((slot == code[0][None, :]) | (slot == code[1][None, :])).astype(BF16)
    outgoing = (
        jnp.dot(chosen, normed, preferred_element_type=F32)
        .astype(BF16)
        .reshape(n_experts, share, width)
    )
    slots = jnp.arange(n_experts * rows, dtype=jnp.int32)[:, None]
    combine = (
        jnp.where(slots == code[0][None, :], route_weight[None, :, 0], 0.0)
        + jnp.where(slots == code[1][None, :], route_weight[None, :, 1], 0.0)
    ).astype(BF16).reshape(n_experts, rows, tokens)

    positions = lax.axis_index("ep") * length + jnp.arange(length, dtype=jnp.int32)
    half = dk // 2
    frequency = theta_base ** (-jnp.arange(half, dtype=F32) / half)
    angles = positions.astype(F32)[:, None] * frequency
    cosine, sine = jnp.cos(angles), jnp.sin(angles)
    cosine = jnp.concatenate([cosine, cosine], axis=1)
    sine = jnp.concatenate([-sine, sine], axis=1)
    running = jnp.cumsum(log_decay, axis=1)

    wide = 512
    sizes = (n_ep, n_tp, heads, dk, dv)
    any_spec = pl.BlockSpec(memory_space=pl.ANY)
    vmem = pl.BlockSpec(memory_space=pltpu.VMEM)
    dma = pltpu.SemaphoreType.DMA
    mixer_out, expert_out = pl.pallas_call(
        functools.partial(kernel, sizes),
        out_shape=(
            jax.ShapeDtypeStruct((length // n_tp, width), BF16),
            jax.ShapeDtypeStruct((tokens, cols), BF16),
        ),
        in_specs=[any_spec] * 15,
        out_specs=(vmem, vmem),
        scratch_shapes=[
            pltpu.VMEM((n_ep, n_tp, share, width), BF16),
            pltpu.VMEM((width, 2 * units), BF16),
            pltpu.VMEM((n_tp, units, cols), BF16),
            pltpu.VMEM((n_experts, rows, tokens), BF16),
            pltpu.VMEM((n_ep, n_tp, rows, units), BF16),
            pltpu.VMEM((n_ep, rows, cols), BF16),
            pltpu.VMEM((n_ep, rows, cols), BF16),
            pltpu.VMEM((length, heads * dk), BF16),
            pltpu.VMEM((length, heads * dk), BF16),
            pltpu.VMEM((length, heads * dv), BF16),
            pltpu.VMEM((length, heads * dv), BF16),
            pltpu.VMEM((length, dk), F32),
            pltpu.VMEM((length, dk), F32),
            pltpu.VMEM((heads, length, 1), F32),
            pltpu.VMEM((heads, 1, length), F32),
            pltpu.VMEM((1, heads * dv), F32),
            pltpu.VMEM((2, heads * dv, wide), BF16),
            pltpu.VMEM((heads, length, dk), BF16),
            pltpu.VMEM((heads, length, dk), BF16),
            pltpu.VMEM((heads, length, dk), BF16),
            pltpu.VMEM((heads, length, dk), BF16),
            pltpu.VMEM((heads, dk, dv), F32),
            pltpu.VMEM((heads, dk, dv), BF16),
            pltpu.VMEM((heads, dk, dv), BF16),
            pltpu.VMEM((heads, length, dv), F32),
            pltpu.VMEM((length, heads * dv), BF16),
            pltpu.VMEM((n_tp, length // n_tp, width), BF16),
            pltpu.VMEM((2, length // n_tp, width), BF16),
            pltpu.VMEM((length // n_tp, width), BF16),
            pltpu.VMEM((tokens, cols), F32),
            dma((12,)),
            dma((2,)),
            dma((n_ep,)), dma((n_ep,)),
            dma((n_ep, 3)), dma((n_ep, 3)),
            dma((n_ep, 3)), dma((n_ep, 3)),
            dma((n_ep,)), dma((n_ep,)),
            dma((n_tp,)), dma((n_tp,)),
            dma, dma,
            dma((3,)), dma((3,)),
        ],
        compiler_params=pltpu.CompilerParams(
            collective_id=0, has_side_effects=True, vmem_limit_bytes=67_043_328
        ),
        name="fused",
    )(
        outgoing, expert_gate, expert_up, expert_down, combine,
        queries, key_rows, value_rows, gate_rows, cosine, sine,
        running[:, :, None], running[:, None, :], head_gain[None, :], out_weight,
    )
    return (mixer_out, expert_out)


def solution(mesh):
    placed = (
        P("ep", "tp"),
        P("ep", "tp"),
        P("ep", "tp"),
        P("ep", "tp"),
        P("tp", "ep"),
        P("tp"),
        P("tp", None),
        P("ep", None),
        P(),
        P("ep", None),
        P("ep", None),
        P("ep", None, "tp"),
        P("ep", None, "tp"),
        P("ep", "tp", None),
    )
    return jax.shard_map(
        body,
        mesh=mesh,
        in_specs=placed,
        out_specs=(P(("ep", "tp"), None), P("ep", "tp")),
        check_vma=False,
    )
```

```python
import functools
import math

import jax
import jax.numpy as jnp
import numpy as np
from jax import lax
from jax.experimental import pallas as pl
from jax.experimental.pallas import tpu as pltpu
from jax.sharding import PartitionSpec as P

MESH = pl.DeviceIdType.MESH
F32, BF16 = jnp.float32, jnp.bfloat16
epsilon = 1e-06
theta_base = 10000.0
LAG = 2
NEAR = 2
WHOLE = 2


def xor(a, b, bits):
    total = 0
    for bit in range(bits):
        step = 1 << bit
        total = total + step * (((a // step) + (b // step)) % 2)
    return total


def dot(a, b, dims=((1,), (0,))):
    return lax.dot_general(a, b, (dims, ((), ())), preferred_element_type=F32)


NT = ((1,), (1,))
TN = ((0,), (0,))


def silu(g):
    return g / (1.0 + jnp.exp(-g))


def kernel(
    sizes,
    expert_in, in_gain, ids, weights, gate, up, down,
    queries, keys, values, gates, cos_near, sin_near, cos_base, sin_base, decay, gain, out_weight,
    mixer_out, expert_out,
    xp, ig_s, ids_s, w_s, code_s, sel, outg, tok, oth, gu, dn, inn_a, inn_b, res_a, res_b, theirs, merged, ret,
    counts, count_out,
    q_in, k_in, v_in, g_in, cos_s, sin_s, cb_s, sb_s, ld_s, rc_s, rr_s, gain_s, ow,
    qhi, qlo, khi, klo, state, carry, packed, even_out, even_in, end_out, end_in, mixed, hidden, from_sib, from_far,
    load_sem, ow_sem,
    disp_s, disp_r, cnt_s, cnt_r, tok_s, tok_r, y_s, y_r, yf_s, yf_r,
    ia_s, ia_r, ib_s, ib_r, mg_s, mg_r, ret_s, ret_r, dn_s, dn_r,
    chain_s, chain_r, even_s, even_r, mix_s, mix_r,
):
    n_ep, n_tp, heads, dk, dv = sizes
    pairs = n_ep // 2
    ep_bits, pair_bits = int(math.log2(n_ep)), int(math.log2(pairs))
    ep = lax.axis_index("ep")
    tp = lax.axis_index("tp")
    pair, par = ep // 2, ep % 2
    mate = xor(ep, 1, 1) + pair * 2
    sib = xor(tp, 1, 2)
    far = xor(tp, 2, 2)
    diag = xor(tp, 3, 2)
    length = queries.shape[0]
    tokens, width = expert_in.shape[0] * expert_in.shape[1], expert_in.shape[2]
    block = tok.shape[1]
    chunk = block // n_tp
    cap = oth.shape[1]
    units = gate.shape[2]
    cols = width // n_tp
    wide = ow.shape[2]
    n_wide = width // wide
    half = width // 2
    side = pl.ds(pl.multiple_of((tp % 2) * half, half), half)
    mine = pl.ds(pl.multiple_of(par * chunk, chunk), cap)
    needed = pl.ds(pl.multiple_of((1 - par) * chunk, chunk), cap)

    def local(k, src, dst):
        return pltpu.make_async_copy(src, dst, load_sem.at[k])

    def remote(src, dst, send, recv, device):
        return pltpu.make_async_remote_copy(
            src_ref=src, dst_ref=dst, send_sem=send, recv_sem=recv,
            device_id=device, device_id_type=MESH,
        )

    def peer_of(m):
        return xor(pair, m, pair_bits)

    outer = (pair == 0) | (pair == pairs - 1)

    def block_at(i):
        late = jnp.where(i == pairs - 1, 1, i + 1)
        return jnp.where(i == 0, 0, jnp.where(outer, late, jnp.where(i == 1, 1, pairs + 1 - i)))

    def send_order(i):
        return jnp.where((i < 2) | ~outer, i, pairs + 1 - i)

    def rows_of(piece):
        return pl.ds(pl.multiple_of(piece * chunk, chunk), chunk)

    def lanes_of(hv):
        return slice(hv * half, (hv + 1) * half)

    def dispatch(m, which, hv):
        return remote(
            outg.at[m + which * pairs, :, lanes_of(hv)],
            tok.at[m, rows_of((tp, far)[which]), lanes_of(hv)],
            disp_s.at[m, which, hv], disp_r.at[m, which, hv], (peer_of(m) * 2 + par, tp),
        )

    def own_rows(which, hv):
        return pltpu.make_async_copy(
            outg.at[which * pairs, :, lanes_of(hv)],
            tok.at[0, rows_of((tp, far)[which]), lanes_of(hv)], disp_r.at[0, which, hv],
        )

    def count_copy(m):
        return remote(count_out, counts.at[m], cnt_s.at[m], cnt_r.at[m], (xor(ep, m, ep_bits), tp))

    def trade_tok(m, kind, hv, incoming=False):
        piece = rows_of(((far, sib, diag) if incoming else (tp, tp, far))[kind])
        device = (ep, (far, sib, sib)[kind])
        there = tok.at[m, piece, lanes_of(hv)]
        return remote(there, there, tok_s.at[m, kind, hv], tok_r.at[m, kind, hv], device)

    def trade(ref, send, recv, m, kind, incoming=False):
        piece = ((far, sib, diag) if incoming else (tp, tp, far))[kind]
        device = (ep, (far, sib, sib)[kind])
        return remote(ref.at[m, piece], ref.at[m, piece], send.at[m, kind], recv.at[m, kind], device)

    def cross(m):
        return remote(tok.at[m, needed, side], oth.at[m, :, side], y_s.at[m], y_r.at[m], (mate, tp))

    def cross_on(m, incoming=False):
        if incoming:
            there = pl.ds(pl.multiple_of((1 - tp % 2) * half, half), half)
        else:
            there = side
        return remote(oth.at[m, :, there], oth.at[m, :, there], yf_s.at[m, 0], yf_r.at[m, 0], (ep, sib))

    def quarter(piece):
        return pl.ds(pl.multiple_of(piece * cols, cols), cols)

    def cross_part(m):
        there = quarter(tp)
        return remote(
            tok.at[m, needed, there], oth.at[m, :, there], y_s.at[m], y_r.at[m], (mate, tp)
        )

    def share(m, kind, incoming=False):
        there = oth.at[m, :, quarter(((far, sib, diag) if incoming else (tp, tp, far))[kind])]
        device = (ep, (far, sib, sib)[kind])
        return remote(there, there, yf_s.at[m, kind], yf_r.at[m, kind], device)

    def to_mate(m):
        return remote(res_b.at[m], theirs.at[m], mg_s.at[m], mg_r.at[m], (mate, tp))

    def give_back(m):
        return remote(merged.at[m], ret.at[m], ret_s.at[m], ret_r.at[m], (peer_of(m) * 2 + par, tp))

    def dn_copy(j, incoming=False):
        peer = xor(tp, j, 2)
        start = pl.multiple_of(peer * cols, cols)
        return remote(
            down.at[0, :, pl.ds(start, cols)], dn.at[peer if incoming else tp],
            dn_s.at[j], dn_r.at[j], (ep, peer),
        )

    def dn_own():
        start = pl.multiple_of(tp * cols, cols)
        return pltpu.make_async_copy(down.at[0, :, pl.ds(start, cols)], dn.at[tp], dn_r.at[0])

    def chain(k):
        return remote(packed, carry, chain_s.at[k], chain_r, ((pair + 1) * 2 + k, tp))

    def even_copies():
        return (
            remote(even_out, even_in, even_s.at[0], even_r.at[0], (mate, tp)),
            remote(end_out, end_in, even_s.at[1], even_r.at[1], (mate, tp)),
        )

    def ow_copy(j, slot):
        start = pl.multiple_of(j * wide, wide)
        return pltpu.make_async_copy(out_weight.at[:, pl.ds(start, wide)], ow.at[slot], ow_sem.at[slot])

    def mix_copy(kind):
        if kind == 0:
            return remote(xp.at[sib], from_sib.at[0], mix_s.at[0], mix_r.at[0], (ep, sib))
        if kind == 1:
            return remote(xp.at[diag], from_sib.at[1], mix_s.at[1], mix_r.at[1], (ep, sib))
        return remote(xp.at[far], from_far, mix_s.at[2], mix_r.at[2], (ep, far))

    loads = [
        local(0, queries, q_in), local(1, keys, k_in), local(2, values, v_in),
        local(3, gates, g_in), local(4, cos_near, cos_s), local(5, sin_near, sin_s),
        local(6, cos_base, cb_s), local(7, sin_base, sb_s), local(8, decay, ld_s),
        local(9, gain, gain_s),
        local(10, gate.at[0], gu.at[:, pl.ds(0, units)]),
        local(11, up.at[0], gu.at[:, pl.ds(units, units)]),
        local(12, expert_in, xp), local(13, in_gain, ig_s), local(14, ids, ids_s),
        local(15, weights, w_s),
    ]

    def begin_retention():
        for k in (0, 1, 2, 4, 5, 6, 7, 8):
            loads[k].wait()
        older = lax.broadcasted_iota(jnp.int32, (length, length), 0)
        newer = lax.broadcasted_iota(jnp.int32, (length, length), 1)
        upper = (older <= newer).astype(BF16)
        lower = (newer <= older).astype(BF16)
        left = ld_s[...]
        run_row = jnp.zeros((heads, length), F32)
        run_col = jnp.zeros((length, heads), F32)
        for _ in range(3):
            piece = left.astype(BF16)
            run_row = run_row + dot(piece, upper)
            run_col = run_col + dot(lower, piece, NT)
            left = left - piece.astype(F32)
        lane = lax.broadcasted_iota(jnp.int32, (1, dk), 1)
        sign = jnp.where(lane < dk // 2, -1.0, 1.0)
        near_cos, near_sin = cos_s[...], sin_s[...]
        base_cos, base_sin = cb_s[ep], sb_s[ep]
        cosine = near_cos * base_cos - near_sin * base_sin
        sine = (near_sin * base_cos + near_cos * base_sin) * sign

        def turn(x):
            return x * cosine + pltpu.roll(x, dk // 2, 1) * sine

        scale = dk ** -0.5
        for h in range(heads):
            lanes = slice(h * dk, (h + 1) * dk)
            q = turn(q_in[:, lanes].astype(F32))
            high = q.astype(BF16)
            qhi[h] = high
            qlo[h] = (q - high.astype(F32)).astype(BF16)
            k = turn(k_in[:, lanes].astype(F32)) * scale
            high = k.astype(BF16)
            khi[h] = high
            klo[h] = (k - high.astype(F32)).astype(BF16)
            col = run_col[:, h : h + 1]
            rc_s[h] = col
            rr_s[h] = run_row[h : h + 1]
            ending = col[length - 1 : length]
            kept = (k * jnp.exp(ending - col)).astype(BF16)
            local_state = dot(kept, v_in[:, h * dv : (h + 1) * dv], TN)
            state[h] = local_state
            even_out[h] = local_state.astype(BF16)
            end_out[h : h + 1] = jnp.broadcast_to(ending, (1, 128))

    barrier = pltpu.get_barrier_semaphore()

    @pl.loop(1, n_ep)
    def _(m):
        pl.semaphore_signal(
            barrier, inc=1, device_id=(xor(ep, m, ep_bits), tp), device_id_type=MESH
        )

    @pl.loop(1, n_tp)
    def _(j):
        pl.semaphore_signal(barrier, inc=1, device_id=(ep, xor(tp, j, 2)), device_id_type=MESH)

    for k in (14, 13, 12, 15, 8, 0, 1, 2, 4, 5, 6, 7):
        loads[k].start()
    dn_own().start()
    for k in (10, 11, 3, 9):
        loads[k].start()
    for j in range(2):
        ow_copy(j, j).start()

    loads[14].wait()
    lanes = lax.broadcasted_iota(jnp.int32, (tokens, 128), 1)
    named = [(ids_s[:, k : k + 1] == lanes).astype(F32) for k in range(2)]
    both = named[0] + named[1]
    order = lax.broadcasted_iota(jnp.int32, (tokens, tokens), 0)
    before = lax.broadcasted_iota(jnp.int32, (tokens, tokens), 1)
    ranks = dot((before < order).astype(BF16), both.astype(BF16))
    total = jnp.sum(both, axis=0, keepdims=True)
    count_out[...] = jnp.broadcast_to(total, count_out.shape)
    code = []
    for k in range(2):
        rank = jnp.sum(named[k] * ranks, axis=1, keepdims=True)
        e = ids_s[:, k : k + 1]
        lower = jnp.where((lanes + 1 == e) & (e % 2 == 1), 1.0, 0.0)
        ahead = jnp.sum(lower * total, axis=1, keepdims=True)
        code.append((e // 2).astype(F32) * block + rank + ahead)
    code_s[...] = jnp.where(lanes == 0, code[0], jnp.where(lanes == 1, code[1], 0.0))
    flipped = code_s[...].T
    slot = lax.broadcasted_iota(jnp.int32, (chunk, 1), 0)
    for n in range(pairs + NEAR):
        first = peer_of(n % pairs) * block + (tp, far)[n // pairs] * chunk
        at = (slot + first).astype(F32)
        sel[n] = ((at == flipped[0:1]) | (at == flipped[1:2])).astype(BF16)

    begin_retention()
    pl.semaphore_wait(barrier, n_ep - 1 + n_tp - 1)

    @pl.when(par == 0)
    def _():
        for copy in even_copies():
            copy.start()

    for j in range(1, n_tp):
        dn_copy(j).start()

    @pl.loop(1, n_ep)
    def _(m):
        count_copy(m).start()

    counts[0] = count_out[...]
    loads[13].wait()
    loads[12].wait()
    part_rows = xp.shape[1]
    step = min(part_rows, 32)

    for part in range(n_tp):

        @pl.loop(0, part_rows // step)
        def _(c):
            at = pl.ds(pl.multiple_of(c * step, step), step)
            x = xp[part, at].astype(F32)
            scale = lax.rsqrt(jnp.mean(x * x, axis=1, keepdims=True) + epsilon)
            xp[part, at] = (x * scale * ig_s[...]).astype(BF16)

    @pl.loop(0, n_wide)
    def _(j):
        here = pl.ds(pl.multiple_of(j * wide, wide), wide)
        rows = xp[:, :, here].reshape(tokens, wide)
        chosen = sel[...].reshape((pairs + NEAR) * chunk, tokens)
        outg[:, :, here] = dot(chosen, rows).astype(BF16).reshape(pairs + NEAR, chunk, wide)

    for hv in range(2):
        for which in range(2):
            own_rows(which, hv).start()

    @pl.loop(1, pairs)
    def _(i):
        m = send_order(i)
        for hv in range(2):
            dispatch(m, 0, hv).start()

            @pl.when(m < NEAR)
            def _():
                dispatch(m, 1, hv).start()

    def pass_state():
        for copy in even_copies():
            copy.wait_recv()
        for h in range(heads):
            last = rc_s[h][length - 1 : length]
            first = end_in[h : h + 1, 0:1]
            earlier = carry[h].astype(F32)
            before = even_in[h].astype(F32)
            packed[h] = (
                jnp.exp(first + last) * earlier + jnp.exp(last) * before + state[h]
            ).astype(BF16)
            carry[h] = (jnp.exp(first) * earlier + before).astype(BF16)

        @pl.when(pair < pairs - 1)
        def _():
            chain(0).start()
            chain(1).start()

    def take_state():
        @pl.when(pair > 0)
        def _():
            chain(0).wait_recv()

        @pl.when(par == 1)
        def _():
            pass_state()

    def inside(h):
        lanes = pl.ds(pl.multiple_of(h * dv, dv), dv)
        vh = v_in[:, lanes]
        col = rc_s[h]
        row = rr_s[h]
        step = min(length, 128)
        for r in range(length // step):
            lines = slice(r * step, (r + 1) * step)
            seen = (r + 1) * step
            score = (
                dot(qhi[h, lines], khi[h, :seen], NT)
                + dot(qhi[h, lines], klo[h, :seen], NT)
                + dot(qlo[h, lines], khi[h, :seen], NT)
            )
            later = lax.broadcasted_iota(jnp.int32, (step, seen), 0) + r * step
            earlier = lax.broadcasted_iota(jnp.int32, (step, seen), 1)
            spread = col[lines] - row[:, :seen]
            weight = jnp.exp(jnp.where(later >= earlier, spread, -jnp.inf))
            mixed[lines, lanes] = dot((score * weight).astype(BF16), vh[:seen])

    def finish_retention():
        loads[3].wait()
        loads[9].wait()
        step = min(length, 128)
        parts = length // step

        @pl.loop(0, heads * parts)
        def _(c):
            h = c // parts
            lines = pl.ds(pl.multiple_of((c % parts) * step, step), step)
            lanes = pl.ds(pl.multiple_of(h * dv, dv), dv)
            begun = carry[h]
            outside = dot(qhi[h, lines], begun) + dot(qlo[h, lines], begun)
            o = mixed[lines, lanes] + outside * jnp.exp(rc_s[h, lines])
            centered = o - jnp.mean(o, axis=1, keepdims=True)
            normed = (
                centered
                * lax.rsqrt(jnp.mean(centered * centered, axis=1, keepdims=True) + epsilon)
                * gain_s[:, lanes]
            )
            hidden[lines, lanes] = (silu(g_in[lines, lanes].astype(F32)) * normed).astype(BF16)

        @pl.loop(0, n_wide)
        def _(j):
            slot = j % 2
            ow_copy(j, slot).wait()
            total = dot(hidden[...], ow[slot]).astype(BF16)
            here = pl.ds(pl.multiple_of(j * wide, wide), wide)
            xp[:, :, here] = total.reshape(n_tp, length // n_tp, wide)

            @pl.when(j + 2 < n_wide)
            def _():
                ow_copy(j + 2, slot).start()

        mix_copy(1).start()
        mix_copy(0).start()

    def forward_mix():
        mix_copy(1).wait_send()
        mix_copy(1).wait_recv()
        xp[far] = (xp[far].astype(F32) + from_sib[1].astype(F32)).astype(BF16)
        mix_copy(2).start()

    line = lax.broadcasted_iota(jnp.int32, (cap, 1), 0).astype(F32) + (par * chunk).astype(F32)
    odd = par.astype(F32)

    def hide(rows, m, other):
        both = dot(rows, gu[...])
        inner = silu(both[:, :units]) * both[:, units:]
        source = 2 * m + other
        tile = counts[source][0:1]
        lane = lax.broadcasted_iota(jnp.int32, tile.shape, 1)
        even = jnp.sum(jnp.where(lane == 2 * pair, tile, 0.0), axis=1, keepdims=True)
        keep = (line < even).astype(F32)
        keep = keep * (1.0 - 2.0 * odd) + odd
        return jnp.where(keep > 0.5, inner, 0.0).astype(BF16)

    def finish(inn, m):
        total = dot(inn[m, 0], dn[0])
        for t in range(1, n_tp):
            total = total + dot(inn[m, t], dn[t])
        return total.astype(BF16)

    def arrive(m):
        for hv in range(2):
            @pl.when(m > 0)
            def _():
                dispatch(m, 0, hv).wait_recv()

            @pl.when(m == 0)
            def _():
                own_rows(0, hv).wait()
                own_rows(1, hv).wait()

            @pl.when(m >= NEAR)
            def _():
                trade_tok(m, 0, hv).start()

            trade_tok(m, 1, hv).start()

            @pl.when((m > 0) & (m < NEAR))
            def _():
                dispatch(m, 1, hv).wait_recv()

            @pl.when(m < NEAR)
            def _():
                trade_tok(m, 2, hv).start()

    def merge(m):
        to_mate(m).wait_recv()

        @pl.when(par == 0)
        def _():
            merged[m, :chunk] = res_a[m, :chunk]
            merged[m, chunk:cap] = res_a[m, chunk:] + theirs[m, : cap - chunk]
            merged[m, cap:] = theirs[m, cap - chunk :]

        @pl.when(par == 1)
        def _():
            merged[m, :chunk] = theirs[m, :chunk]
            merged[m, chunk:cap] = theirs[m, chunk:] + res_a[m, : cap - chunk]
            merged[m, cap:] = res_a[m, cap - chunk :]

        @pl.when(m > 0)
        def _():
            give_back(m).start()

    def spread(m, hv, late):
        @pl.when(m >= NEAR)
        def _():
            trade_tok(m, 0, hv, True).wait_recv()
            trade_tok(m, 2, hv).start()

        trade_tok(m, 1, hv, True).wait_recv()
        trade_tok(m, 2, hv, True).wait_recv()

        @pl.when(jnp.logical_not(late) & (tp % 2 == hv))
        def _():
            cross(m).start()

        @pl.when(late & (tp // 2 == hv))
        def _():
            cross_part(m).start()

    arrive(jnp.int32(0))

    @pl.loop(0, pairs + LAG)
    def _(i):
        @pl.when(i < pairs)
        def _():
            m = block_at(i)
            spread(m, 0, i >= WHOLE)
            spread(m, 1, i >= WHOLE)

            @pl.when(i == 0)
            def _():
                loads[10].wait()
                loads[11].wait()

            @pl.when(m > 0)
            def _():
                count_copy(2 * m).wait_recv()

            inn_a[m, tp] = hide(tok[m, mine], m, 0)
            trade(inn_a, ia_s, ia_r, m, 0).start()
            trade(inn_a, ia_s, ia_r, m, 1).start()

        @pl.when(i == 0)
        def _():
            @pl.when(pair == 0)
            def _():
                carry[...] = jnp.zeros_like(carry)

            @pl.loop(0, heads)
            def _(h):
                inside(h)

        @pl.when(((i == 0) & (pair == 0)) | ((i == pair + 1) & (pair > 0) & (pair < pairs - 1)))
        def _():
            take_state()

        @pl.when((i - 1 >= WHOLE) & (i < pairs + 1))
        def _():
            m = block_at(i - 1)
            cross_part(m).wait_recv()
            share(m, 0).start()
            share(m, 1).start()

        @pl.when(i < pairs - 1)
        def _():
            arrive(block_at(i + 1))

        @pl.when(i == pairs - 1)
        def _():
            @pl.when(pair == pairs - 1)
            def _():
                take_state()

            finish_retention()

        @pl.when(i == pairs)
        def _():
            merge(block_at(i - 2))

        @pl.when(i == 1)
        def _():
            dn_own().wait()
            for j in range(1, n_tp):
                dn_copy(j, True).wait_recv()

        @pl.when((i >= 1) & (i < pairs + 1))
        def _():
            m = block_at(i - 1)
            trade(inn_a, ia_s, ia_r, m, 0, True).wait_recv()
            trade(inn_a, ia_s, ia_r, m, 2).start()

            @pl.when(i - 1 < WHOLE)
            def _():
                cross(m).wait_recv()
                cross_on(m).start()
                cross_on(m, True).wait_recv()

            @pl.when(i - 1 >= WHOLE)
            def _():
                share(m, 0, True).wait_recv()
                share(m, 2).start()
                share(m, 1, True).wait_recv()
                share(m, 2, True).wait_recv()

            count_copy(2 * m + 1).wait_recv()
            inn_b[m, tp] = hide(oth[m], m, 1)
            trade(inn_b, ib_s, ib_r, m, 0).start()
            trade(inn_b, ib_s, ib_r, m, 1).start()

            @pl.when(i == pairs)
            def _():
                forward_mix()

            trade(inn_a, ia_s, ia_r, m, 1, True).wait_recv()
            trade(inn_a, ia_s, ia_r, m, 2, True).wait_recv()
            res_a[m] = finish(inn_a, m)
            trade(inn_b, ib_s, ib_r, m, 0, True).wait_recv()
            trade(inn_b, ib_s, ib_r, m, 2).start()
            trade(inn_b, ib_s, ib_r, m, 1, True).wait_recv()
            trade(inn_b, ib_s, ib_r, m, 2, True).wait_recv()
            res_b[m] = finish(inn_b, m)
            to_mate(m).start()

        @pl.when((i >= 2) & (i != pairs))
        def _():
            merge(block_at(i - 2))

    loads[15].wait()
    place = lax.broadcasted_iota(jnp.int32, (tokens, block), 1).astype(F32)

    def combine(m, rows):
        at = code_s[...] - (peer_of(m) * block).astype(F32)
        pick = jnp.where(place == at[:, 0:1], w_s[:, 0:1], 0.0) + jnp.where(
            place == at[:, 1:2], w_s[:, 1:2], 0.0
        )
        return dot(pick.astype(BF16), rows)

    mixed[...] = combine(0, merged[0])

    mix_copy(0).wait_recv()
    mix_copy(2).wait_recv()
    mixer_out[...] = (
        xp[tp].astype(F32) + from_sib[0].astype(F32) + from_far[...].astype(F32)
    ).astype(BF16)

    @pl.loop(0, pairs - 1)
    def _(i):
        m = block_at(i + 1)
        give_back(m).wait_recv()
        mixed[...] += combine(m, ret[m])

    expert_out[...] = mixed[...].astype(BF16)

    mix_copy(0).wait_send()
    mix_copy(2).wait_send()

    @pl.when((par == 1) & (pair < pairs - 1))
    def _():
        chain(0).wait_send()
        chain(1).wait_send()

    @pl.when(par == 0)
    def _():
        for copy in even_copies():
            copy.wait_send()

    for j in range(1, n_tp):
        dn_copy(j).wait_send()

    @pl.loop(0, pairs)
    def _(i):
        m = block_at(i)
        for hv in range(2):
            @pl.when(m >= NEAR)
            def _():
                trade_tok(m, 0, hv).wait_send()

            trade_tok(m, 1, hv).wait_send()
            trade_tok(m, 2, hv).wait_send()

        for kind in range(3):
            trade(inn_a, ia_s, ia_r, m, kind).wait_send()
            trade(inn_b, ib_s, ib_r, m, kind).wait_send()

        @pl.when(i < WHOLE)
        def _():
            cross(m).wait_send()
            cross_on(m).wait_send()

        @pl.when(i >= WHOLE)
        def _():
            cross_part(m).wait_send()
            for kind in range(3):
                share(m, kind).wait_send()

        to_mate(m).wait_send()

    @pl.loop(1, pairs)
    def _(m):
        for hv in range(2):
            dispatch(m, 0, hv).wait_send()

            @pl.when(m < NEAR)
            def _():
                dispatch(m, 1, hv).wait_send()

        give_back(m).wait_send()

    @pl.loop(1, n_ep)
    def _(m):
        count_copy(m).wait_send()


def body(
    queries, key_rows, value_rows, gate_rows, log_decay, head_gain, out_weight,
    expert_input, input_gain, route_ids, route_weight, expert_gate, expert_up, expert_down,
):
    n_tp = lax.axis_size("tp")
    n_ep = lax.axis_size("ep")
    width = out_weight.shape[1]
    tokens = expert_input.shape[0]
    n_experts = n_ep * expert_gate.shape[0]
    units = expert_gate.shape[2]
    capacity = 3 * tokens // n_experts
    block = 4 * capacity // 3
    chunk = block // n_tp
    pairs = n_ep // 2
    cols = width // n_tp
    length = queries.shape[0]
    heads = log_decay.shape[0]
    dk = queries.shape[1] // heads
    dv = value_rows.shape[1] // heads
    assert tokens == length and cols == heads * dv

    half = dk // 2
    frequency = theta_base ** (-np.arange(half) / half)
    frequency = np.concatenate([frequency, frequency])
    near = np.arange(length)[:, None] * frequency
    base = (np.arange(n_ep) * length)[:, None, None] * frequency
    tables = [jnp.asarray(f(a), F32) for a in (near, base) for f in (np.cos, np.sin)]

    wide = 512
    sizes = (n_ep, n_tp, heads, dk, dv)
    any_spec = pl.BlockSpec(memory_space=pl.ANY)
    vmem = pl.BlockSpec(memory_space=pltpu.VMEM)
    dma = pltpu.SemaphoreType.DMA
    V = pltpu.VMEM
    mixer_out, expert_out = pl.pallas_call(
        functools.partial(kernel, sizes),
        out_shape=(
            jax.ShapeDtypeStruct((length // n_tp, width), BF16),
            jax.ShapeDtypeStruct((tokens, cols), BF16),
        ),
        in_specs=[any_spec] * 18,
        out_specs=(vmem, vmem),
        scratch_shapes=[
            V((n_tp, tokens // n_tp, width), BF16),
            V((1, width), F32),
            V((tokens, 2), jnp.int32),
            V((tokens, 2), F32),
            V((tokens, 128), F32),
            V((pairs + NEAR, chunk, tokens), BF16),
            V((pairs + NEAR, chunk, width), BF16),
            V((pairs, block, width), BF16),
            V((pairs, capacity, width), BF16),
            V((width, 2 * units), BF16),
            V((n_tp, units, cols), BF16),
            V((pairs, n_tp, capacity, units), BF16),
            V((pairs, n_tp, capacity, units), BF16),
            V((pairs, capacity, cols), BF16),
            V((pairs, capacity, cols), BF16),
            V((pairs, capacity, cols), BF16),
            V((pairs, block, cols), BF16),
            V((pairs, block, cols), BF16),
            V((n_ep, 8, 128), F32),
            V((8, 128), F32),
            V((length, heads * dk), BF16),
            V((length, heads * dk), BF16),
            V((length, heads * dv), BF16),
            V((length, heads * dv), BF16),
            V((length, dk), F32),
            V((length, dk), F32),
            V((n_ep, 1, dk), F32),
            V((n_ep, 1, dk), F32),
            V((heads, length), F32),
            V((heads, length, 1), F32),
            V((heads, 1, length), F32),
            V((1, heads * dv), F32),
            V((2, heads * dv, wide), BF16),
            V((heads, length, dk), BF16),
            V((heads, length, dk), BF16),
            V((heads, length, dk), BF16),
            V((heads, length, dk), BF16),
            V((heads, dk, dv), F32),
            V((heads, dk, dv), BF16),
            V((heads, dk, dv), BF16),
            V((heads, dk, dv), BF16),
            V((heads, dk, dv), BF16),
            V((8, 128), F32),
            V((8, 128), F32),
            V((length, heads * dv), F32),
            V((length, heads * dv), BF16),
            V((2, length // n_tp, width), BF16),
            V((length // n_tp, width), BF16),
            dma((16,)),
            dma((2,)),
            dma((pairs, 2, 2)), dma((pairs, 2, 2)),
            dma((n_ep,)), dma((n_ep,)),
            dma((pairs, 3, 2)), dma((pairs, 3, 2)),
            dma((pairs,)), dma((pairs,)),
            dma((pairs, 3)), dma((pairs, 3)),
            dma((pairs, 3)), dma((pairs, 3)),
            dma((pairs, 3)), dma((pairs, 3)),
            dma((pairs,)), dma((pairs,)),
            dma((pairs,)), dma((pairs,)),
            dma((n_tp,)), dma((n_tp,)),
            dma((2,)), dma,
            dma((2,)), dma((2,)),
            dma((3,)), dma((3,)),
        ],
        compiler_params=pltpu.CompilerParams(
            collective_id=0, has_side_effects=True, vmem_limit_bytes=67_043_328
        ),
        name="fused",
    )(
        expert_input.reshape(n_tp, tokens // n_tp, width), input_gain[None, :],
        route_ids, route_weight, expert_gate, expert_up, expert_down,
        queries, key_rows, value_rows, gate_rows, tables[0], tables[1], tables[2], tables[3],
        log_decay, head_gain[None, :], out_weight,
    )
    return (mixer_out, expert_out)


def solution(mesh):
    placed = (
        P("ep", "tp"),
        P("ep", "tp"),
        P("ep", "tp"),
        P("ep", "tp"),
        P("tp", "ep"),
        P("tp"),
        P("tp", None),
        P("ep", None),
        P(),
        P("ep", None),
        P("ep", None),
        P("ep", None, "tp"),
        P("ep", None, "tp"),
        P("ep", "tp", None),
    )
    return jax.shard_map(
        body,
        mesh=mesh,
        in_specs=placed,
        out_specs=(P(("ep", "tp"), None), P("ep", "tp")),
        check_vma=False,
    )
```

```python
import functools
import math

import jax
import jax.numpy as jnp
import numpy as np
from jax import lax
from jax.experimental import pallas as pl
from jax.experimental.pallas import tpu as pltpu
from jax.sharding import PartitionSpec as P

MESH = pl.DeviceIdType.MESH
F32, BF16 = jnp.float32, jnp.bfloat16
epsilon = 1e-06
theta_base = 10000.0
LAG = 2
NEAR = 2
WHOLE = 2


def xor(a, b, bits):
    total = 0
    for bit in range(bits):
        step = 1 << bit
        total = total + step * (((a // step) + (b // step)) % 2)
    return total


def dot(a, b, dims=((1,), (0,))):
    return lax.dot_general(a, b, (dims, ((), ())), preferred_element_type=F32)


NT = ((1,), (1,))
TN = ((0,), (0,))


def silu(g):
    return g / (1.0 + jnp.exp(-g))


def kernel(
    sizes,
    expert_in, in_gain, ids, weights, gate, up, down,
    queries, keys, values, gates, cos_near, sin_near, cos_base, sin_base, decay, gain, out_weight,
    mixer_out, expert_out,
    xp, ig_s, ids_s, w_s, code_s, sel, outg, tok, oth, gu, dn, inn_a, inn_b, res_a, res_b, theirs, merged, ret,
    counts, count_out,
    q_in, k_in, v_in, g_in, cos_s, sin_s, cb_s, sb_s, ld_s, rc_s, rr_s, gain_s, ow,
    qhi, qlo, khi, klo, state, carry, packed, even_out, even_in, end_out, end_in, mixed, hidden, from_sib, from_far,
    load_sem, ow_sem,
    disp_s, disp_r, cnt_s, cnt_r, tok_s, tok_r, y_s, y_r, yf_s, yf_r,
    ia_s, ia_r, ib_s, ib_r, mg_s, mg_r, ret_s, ret_r, dn_s, dn_r,
    chain_s, chain_r, even_s, even_r, mix_s, mix_r,
):
    n_ep, n_tp, heads, dk, dv = sizes
    pairs = n_ep // 2
    ep_bits, pair_bits = int(math.log2(n_ep)), int(math.log2(pairs))
    ep = lax.axis_index("ep")
    tp = lax.axis_index("tp")
    pair, par = ep // 2, ep % 2
    mate = xor(ep, 1, 1) + pair * 2
    sib = xor(tp, 1, 2)
    far = xor(tp, 2, 2)
    diag = xor(tp, 3, 2)
    length = queries.shape[0]
    tokens, width = expert_in.shape[0] * expert_in.shape[1], expert_in.shape[2]
    block = tok.shape[1]
    chunk = block // n_tp
    cap = oth.shape[1]
    units = gate.shape[2]
    cols = width // n_tp
    wide = ow.shape[2]
    n_wide = width // wide
    half = width // 2
    side = pl.ds(pl.multiple_of((tp % 2) * half, half), half)
    mine = pl.ds(pl.multiple_of(par * chunk, chunk), cap)
    needed = pl.ds(pl.multiple_of((1 - par) * chunk, chunk), cap)

    def local(k, src, dst):
        return pltpu.make_async_copy(src, dst, load_sem.at[k])

    def remote(src, dst, send, recv, device):
        return pltpu.make_async_remote_copy(
            src_ref=src, dst_ref=dst, send_sem=send, recv_sem=recv,
            device_id=device, device_id_type=MESH,
        )

    def peer_of(m):
        return xor(pair, m, pair_bits)

    outer = (pair == 0) | (pair == pairs - 1)

    def block_at(i):
        late = jnp.where(i == pairs - 1, 1, i + 1)
        return jnp.where(i == 0, 0, jnp.where(outer, late, jnp.where(i == 1, 1, pairs + 1 - i)))

    def send_order(i):
        return jnp.where((i < 2) | ~outer, i, pairs + 1 - i)

    def rows_of(piece):
        return pl.ds(pl.multiple_of(piece * chunk, chunk), chunk)

    def lanes_of(hv):
        return slice(hv * half, (hv + 1) * half)

    def dispatch(m, which, hv):
        return remote(
            outg.at[m + which * pairs, :, lanes_of(hv)],
            tok.at[m, rows_of((tp, far)[which]), lanes_of(hv)],
            disp_s.at[m, which, hv], disp_r.at[m, which, hv], (peer_of(m) * 2 + par, tp),
        )

    def own_rows(which, hv):
        return pltpu.make_async_copy(
            outg.at[which * pairs, :, lanes_of(hv)],
            tok.at[0, rows_of((tp, far)[which]), lanes_of(hv)], disp_r.at[0, which, hv],
        )

    def count_copy(m):
        return remote(count_out, counts.at[m], cnt_s.at[m], cnt_r.at[m], (xor(ep, m, ep_bits), tp))

    def trade_tok(m, kind, hv, incoming=False):
        piece = rows_of(((far, sib, diag) if incoming else (tp, tp, far))[kind])
        device = (ep, (far, sib, sib)[kind])
        there = tok.at[m, piece, lanes_of(hv)]
        return remote(there, there, tok_s.at[m, kind, hv], tok_r.at[m, kind, hv], device)

    def trade(ref, send, recv, m, kind, incoming=False):
        piece = ((far, sib, diag) if incoming else (tp, tp, far))[kind]
        device = (ep, (far, sib, sib)[kind])
        return remote(ref.at[m, piece], ref.at[m, piece], send.at[m, kind], recv.at[m, kind], device)

    def cross(m):
        return remote(tok.at[m, needed, side], oth.at[m, :, side], y_s.at[m], y_r.at[m], (mate, tp))

    def cross_on(m, incoming=False):
        if incoming:
            there = pl.ds(pl.multiple_of((1 - tp % 2) * half, half), half)
        else:
            there = side
        return remote(oth.at[m, :, there], oth.at[m, :, there], yf_s.at[m, 0], yf_r.at[m, 0], (ep, sib))

    def quarter(piece):
        return pl.ds(pl.multiple_of(piece * cols, cols), cols)

    def cross_part(m):
        there = quarter(tp)
        return remote(
            tok.at[m, needed, there], oth.at[m, :, there], y_s.at[m], y_r.at[m], (mate, tp)
        )

    def share(m, kind, incoming=False):
        there = oth.at[m, :, quarter(((far, sib, diag) if incoming else (tp, tp, far))[kind])]
        device = (ep, (far, sib, sib)[kind])
        return remote(there, there, yf_s.at[m, kind], yf_r.at[m, kind], device)

    def to_mate(m):
        return remote(res_b.at[m], theirs.at[m], mg_s.at[m], mg_r.at[m], (mate, tp))

    def give_back(m):
        return remote(merged.at[m], ret.at[m], ret_s.at[m], ret_r.at[m], (peer_of(m) * 2 + par, tp))

    def dn_copy(j, incoming=False):
        peer = xor(tp, j, 2)
        start = pl.multiple_of(peer * cols, cols)
        return remote(
            down.at[0, :, pl.ds(start, cols)], dn.at[peer if incoming else tp],
            dn_s.at[j], dn_r.at[j], (ep, peer),
        )

    def dn_own():
        start = pl.multiple_of(tp * cols, cols)
        return pltpu.make_async_copy(down.at[0, :, pl.ds(start, cols)], dn.at[tp], dn_r.at[0])

    def chain(k):
        return remote(packed, carry, chain_s.at[k], chain_r, ((pair + 1) * 2 + k, tp))

    def even_copies():
        return (
            remote(even_out, even_in, even_s.at[0], even_r.at[0], (mate, tp)),
            remote(end_out, end_in, even_s.at[1], even_r.at[1], (mate, tp)),
        )

    def ow_copy(j, slot):
        start = pl.multiple_of(j * wide, wide)
        return pltpu.make_async_copy(out_weight.at[:, pl.ds(start, wide)], ow.at[slot], ow_sem.at[slot])

    def mix_copy(kind):
        if kind == 0:
            return remote(xp.at[sib], from_sib.at[0], mix_s.at[0], mix_r.at[0], (ep, sib))
        if kind == 1:
            return remote(xp.at[diag], from_sib.at[1], mix_s.at[1], mix_r.at[1], (ep, sib))
        return remote(xp.at[far], from_far, mix_s.at[2], mix_r.at[2], (ep, far))

    loads = [
        local(0, queries, q_in), local(1, keys, k_in), local(2, values, v_in),
        local(3, gates, g_in), local(4, cos_near, cos_s), local(5, sin_near, sin_s),
        local(6, cos_base, cb_s), local(7, sin_base, sb_s), local(8, decay, ld_s),
        local(9, gain, gain_s),
        local(10, gate.at[0], gu.at[:, pl.ds(0, units)]),
        local(11, up.at[0], gu.at[:, pl.ds(units, units)]),
        local(12, expert_in, xp), local(13, in_gain, ig_s), local(14, ids, ids_s),
        local(15, weights, w_s),
    ]

    def begin_retention():
        for k in (0, 1, 2, 4, 5, 6, 7, 8):
            loads[k].wait()
        older = lax.broadcasted_iota(jnp.int32, (length, length), 0)
        newer = lax.broadcasted_iota(jnp.int32, (length, length), 1)
        upper = (older <= newer).astype(BF16)
        lower = (newer <= older).astype(BF16)
        left = ld_s[...]
        run_row = jnp.zeros((heads, length), F32)
        run_col = jnp.zeros((length, heads), F32)
        for _ in range(3):
            piece = left.astype(BF16)
            run_row = run_row + dot(piece, upper)
            run_col = run_col + dot(lower, piece, NT)
            left = left - piece.astype(F32)
        lane = lax.broadcasted_iota(jnp.int32, (1, dk), 1)
        sign = jnp.where(lane < dk // 2, -1.0, 1.0)
        near_cos, near_sin = cos_s[...], sin_s[...]
        base_cos, base_sin = cb_s[ep], sb_s[ep]
        cosine = near_cos * base_cos - near_sin * base_sin
        sine = (near_sin * base_cos + near_cos * base_sin) * sign

        def turn(x):
            return x * cosine + pltpu.roll(x, dk // 2, 1) * sine

        scale = dk ** -0.5
        for h in range(heads):
            lanes = slice(h * dk, (h + 1) * dk)
            q = turn(q_in[:, lanes].astype(F32))
            high = q.astype(BF16)
            qhi[h] = high
            qlo[h] = (q - high.astype(F32)).astype(BF16)
            k = turn(k_in[:, lanes].astype(F32)) * scale
            high = k.astype(BF16)
            khi[h] = high
            klo[h] = (k - high.astype(F32)).astype(BF16)
            col = run_col[:, h : h + 1]
            rc_s[h] = col
            rr_s[h] = run_row[h : h + 1]
            ending = col[length - 1 : length]
            kept = (k * jnp.exp(ending - col)).astype(BF16)
            local_state = dot(kept, v_in[:, h * dv : (h + 1) * dv], TN)
            state[h] = local_state
            even_out[h] = local_state.astype(BF16)
            end_out[h : h + 1] = jnp.broadcast_to(ending, (1, 128))

    barrier = pltpu.get_barrier_semaphore()

    @pl.loop(1, n_ep)
    def _(m):
        pl.semaphore_signal(
            barrier, inc=1, device_id=(xor(ep, m, ep_bits), tp), device_id_type=MESH
        )

    @pl.loop(1, n_tp)
    def _(j):
        pl.semaphore_signal(barrier, inc=1, device_id=(ep, xor(tp, j, 2)), device_id_type=MESH)

    for k in (14, 13, 12, 15, 8, 0, 1, 2, 4, 5, 6, 7):
        loads[k].start()
    dn_own().start()
    for k in (10, 11, 3, 9):
        loads[k].start()
    for j in range(2):
        ow_copy(j, j).start()

    loads[14].wait()
    lanes = lax.broadcasted_iota(jnp.int32, (tokens, 128), 1)
    named = [(ids_s[:, k : k + 1] == lanes).astype(F32) for k in range(2)]
    both = named[0] + named[1]
    order = lax.broadcasted_iota(jnp.int32, (tokens, tokens), 0)
    before = lax.broadcasted_iota(jnp.int32, (tokens, tokens), 1)
    ranks = dot((before < order).astype(BF16), both.astype(BF16))
    total = jnp.sum(both, axis=0, keepdims=True)
    count_out[...] = jnp.broadcast_to(total, count_out.shape)
    code = []
    for k in range(2):
        rank = jnp.sum(named[k] * ranks, axis=1, keepdims=True)
        e = ids_s[:, k : k + 1]
        lower = jnp.where((lanes + 1 == e) & (e % 2 == 1), 1.0, 0.0)
        ahead = jnp.sum(lower * total, axis=1, keepdims=True)
        code.append((e // 2).astype(F32) * block + rank + ahead)
    code_s[...] = jnp.where(lanes == 0, code[0], jnp.where(lanes == 1, code[1], 0.0))
    flipped = code_s[...].T
    slot = lax.broadcasted_iota(jnp.int32, (chunk, 1), 0)
    for n in range(pairs + NEAR):
        first = peer_of(n % pairs) * block + (tp, far)[n // pairs] * chunk
        at = (slot + first).astype(F32)
        sel[n] = ((at == flipped[0:1]) | (at == flipped[1:2])).astype(BF16)

    begin_retention()
    pl.semaphore_wait(barrier, n_ep - 1 + n_tp - 1)

    @pl.when(par == 0)
    def _():
        for copy in even_copies():
            copy.start()

    for j in range(1, n_tp):
        dn_copy(j).start()

    @pl.loop(1, n_ep)
    def _(m):
        count_copy(m).start()

    counts[0] = count_out[...]
    loads[13].wait()
    loads[12].wait()
    part_rows = xp.shape[1]
    step = min(part_rows, 32)

    for part in range(n_tp):

        @pl.loop(0, part_rows // step)
        def _(c):
            at = pl.ds(pl.multiple_of(c * step, step), step)
            x = xp[part, at].astype(F32)
            scale = lax.rsqrt(jnp.mean(x * x, axis=1, keepdims=True) + epsilon)
            xp[part, at] = (x * scale * ig_s[...]).astype(BF16)

    @pl.loop(0, n_wide)
    def _(j):
        here = pl.ds(pl.multiple_of(j * wide, wide), wide)
        rows = xp[:, :, here].reshape(tokens, wide)
        chosen = sel[...].reshape((pairs + NEAR) * chunk, tokens)
        outg[:, :, here] = dot(chosen, rows).astype(BF16).reshape(pairs + NEAR, chunk, wide)

    for hv in range(2):
        for which in range(2):
            own_rows(which, hv).start()

    @pl.loop(1, pairs)
    def _(i):
        m = send_order(i)
        for hv in range(2):
            dispatch(m, 0, hv).start()

            @pl.when(m < NEAR)
            def _():
                dispatch(m, 1, hv).start()

    def pass_state():
        for copy in even_copies():
            copy.wait_recv()
        for h in range(heads):
            last = rc_s[h][length - 1 : length]
            first = end_in[h : h + 1, 0:1]
            earlier = carry[h].astype(F32)
            before = even_in[h].astype(F32)
            packed[h] = (
                jnp.exp(first + last) * earlier + jnp.exp(last) * before + state[h]
            ).astype(BF16)
            carry[h] = (jnp.exp(first) * earlier + before).astype(BF16)

        @pl.when(pair < pairs - 1)
        def _():
            chain(0).start()
            chain(1).start()

    def inside(h):
        lanes = pl.ds(pl.multiple_of(h * dv, dv), dv)
        vh = v_in[:, lanes]
        col = rc_s[h]
        row = rr_s[h]
        step = min(length, 128)
        for r in range(length // step):
            lines = slice(r * step, (r + 1) * step)
            seen = (r + 1) * step
            score = (
                dot(qhi[h, lines], khi[h, :seen], NT)
                + dot(qhi[h, lines], klo[h, :seen], NT)
                + dot(qlo[h, lines], khi[h, :seen], NT)
            )
            later = lax.broadcasted_iota(jnp.int32, (step, seen), 0) + r * step
            earlier = lax.broadcasted_iota(jnp.int32, (step, seen), 1)
            spread = col[lines] - row[:, :seen]
            weight = jnp.exp(jnp.where(later >= earlier, spread, -jnp.inf))
            mixed[lines, lanes] = dot((score * weight).astype(BF16), vh[:seen])

    def finish_retention():
        loads[3].wait()
        loads[9].wait()
        step = min(length, 128)
        parts = length // step

        @pl.loop(0, heads * parts)
        def _(c):
            h = c // parts
            lines = pl.ds(pl.multiple_of((c % parts) * step, step), step)
            lanes = pl.ds(pl.multiple_of(h * dv, dv), dv)
            begun = carry[h]
            outside = dot(qhi[h, lines], begun) + dot(qlo[h, lines], begun)
            o = mixed[lines, lanes] + outside * jnp.exp(rc_s[h, lines])
            centered = o - jnp.mean(o, axis=1, keepdims=True)
            normed = (
                centered
                * lax.rsqrt(jnp.mean(centered * centered, axis=1, keepdims=True) + epsilon)
                * gain_s[:, lanes]
            )
            hidden[lines, lanes] = (silu(g_in[lines, lanes].astype(F32)) * normed).astype(BF16)

        @pl.loop(0, n_wide)
        def _(j):
            slot = j % 2
            ow_copy(j, slot).wait()
            total = dot(hidden[...], ow[slot]).astype(BF16)
            here = pl.ds(pl.multiple_of(j * wide, wide), wide)
            xp[:, :, here] = total.reshape(n_tp, length // n_tp, wide)

            @pl.when(j + 2 < n_wide)
            def _():
                ow_copy(j + 2, slot).start()

        mix_copy(1).start()
        mix_copy(0).start()

    def forward_mix():
        mix_copy(1).wait_send()
        mix_copy(1).wait_recv()
        xp[far] = (xp[far].astype(F32) + from_sib[1].astype(F32)).astype(BF16)
        mix_copy(2).start()

    line = lax.broadcasted_iota(jnp.int32, (cap, 1), 0).astype(F32) + (par * chunk).astype(F32)
    odd = par.astype(F32)

    def hide(rows, m, other):
        both = dot(rows, gu[...])
        inner = silu(both[:, :units]) * both[:, units:]
        source = 2 * m + other
        tile = counts[source][0:1]
        lane = lax.broadcasted_iota(jnp.int32, tile.shape, 1)
        even = jnp.sum(jnp.where(lane == 2 * pair, tile, 0.0), axis=1, keepdims=True)
        keep = (line < even).astype(F32)
        keep = keep * (1.0 - 2.0 * odd) + odd
        return jnp.where(keep > 0.5, inner, 0.0).astype(BF16)

    def finish(inn, m):
        total = dot(inn[m, 0], dn[0])
        for t in range(1, n_tp):
            total = total + dot(inn[m, t], dn[t])
        return total.astype(BF16)

    def arrive(m):
        for hv in range(2):
            @pl.when(m > 0)
            def _():
                dispatch(m, 0, hv).wait_recv()

            @pl.when(m == 0)
            def _():
                own_rows(0, hv).wait()
                own_rows(1, hv).wait()

            @pl.when(m >= NEAR)
            def _():
                trade_tok(m, 0, hv).start()

            trade_tok(m, 1, hv).start()

            @pl.when((m > 0) & (m < NEAR))
            def _():
                dispatch(m, 1, hv).wait_recv()

            @pl.when(m < NEAR)
            def _():
                trade_tok(m, 2, hv).start()

    def merge(m):
        to_mate(m).wait_recv()

        @pl.when(par == 0)
        def _():
            merged[m, :chunk] = res_a[m, :chunk]
            merged[m, chunk:cap] = res_a[m, chunk:] + theirs[m, : cap - chunk]
            merged[m, cap:] = theirs[m, cap - chunk :]

        @pl.when(par == 1)
        def _():
            merged[m, :chunk] = theirs[m, :chunk]
            merged[m, chunk:cap] = theirs[m, chunk:] + res_a[m, : cap - chunk]
            merged[m, cap:] = res_a[m, cap - chunk :]

        @pl.when(m > 0)
        def _():
            give_back(m).start()

    def spread(m, hv, late):
        @pl.when(m >= NEAR)
        def _():
            trade_tok(m, 0, hv, True).wait_recv()
            trade_tok(m, 2, hv).start()

        trade_tok(m, 1, hv, True).wait_recv()
        trade_tok(m, 2, hv, True).wait_recv()

        @pl.when(jnp.logical_not(late) & (tp % 2 == hv))
        def _():
            cross(m).start()

        @pl.when(late & (tp // 2 == hv))
        def _():
            cross_part(m).start()

    arrive(jnp.int32(0))

    @pl.loop(0, pairs + LAG)
    def _(i):
        @pl.when(i < pairs)
        def _():
            m = block_at(i)
            spread(m, 0, i >= WHOLE)
            spread(m, 1, i >= WHOLE)

            @pl.when(i == 0)
            def _():
                loads[10].wait()
                loads[11].wait()

            @pl.when(m > 0)
            def _():
                count_copy(2 * m).wait_recv()

            inn_a[m, tp] = hide(tok[m, mine], m, 0)
            trade(inn_a, ia_s, ia_r, m, 0).start()
            trade(inn_a, ia_s, ia_r, m, 1).start()

        @pl.when(i == 0)
        def _():
            @pl.when(pair == 0)
            def _():
                carry[...] = jnp.zeros_like(carry)

            @pl.loop(0, heads)
            def _(h):
                inside(h)

        @pl.when(((i == 0) & (pair == 0)) | ((i == pair + 1) & (pair > 0)))
        def _():
            @pl.when(pair > 0)
            def _():
                chain(0).wait_recv()

            @pl.when(par == 1)
            def _():
                pass_state()

        @pl.when((i - 1 >= WHOLE) & (i < pairs + 1))
        def _():
            m = block_at(i - 1)
            cross_part(m).wait_recv()
            share(m, 0).start()
            share(m, 1).start()

        @pl.when(i < pairs - 1)
        def _():
            arrive(block_at(i + 1))

        @pl.when(i == pairs)
        def _():
            finish_retention()
            merge(block_at(i - 2))

        @pl.when(i == 1)
        def _():
            dn_own().wait()
            for j in range(1, n_tp):
                dn_copy(j, True).wait_recv()

        @pl.when((i >= 1) & (i < pairs + 1))
        def _():
            m = block_at(i - 1)
            trade(inn_a, ia_s, ia_r, m, 0, True).wait_recv()
            trade(inn_a, ia_s, ia_r, m, 2).start()

            @pl.when(i - 1 < WHOLE)
            def _():
                cross(m).wait_recv()
                cross_on(m).start()
                cross_on(m, True).wait_recv()

            @pl.when(i - 1 >= WHOLE)
            def _():
                share(m, 0, True).wait_recv()
                share(m, 2).start()
                share(m, 1, True).wait_recv()
                share(m, 2, True).wait_recv()

            count_copy(2 * m + 1).wait_recv()
            inn_b[m, tp] = hide(oth[m], m, 1)
            trade(inn_b, ib_s, ib_r, m, 0).start()
            trade(inn_b, ib_s, ib_r, m, 1).start()

            @pl.when(i == pairs)
            def _():
                forward_mix()

            trade(inn_a, ia_s, ia_r, m, 1, True).wait_recv()
            trade(inn_a, ia_s, ia_r, m, 2, True).wait_recv()
            res_a[m] = finish(inn_a, m)
            trade(inn_b, ib_s, ib_r, m, 0, True).wait_recv()
            trade(inn_b, ib_s, ib_r, m, 2).start()
            trade(inn_b, ib_s, ib_r, m, 1, True).wait_recv()
            trade(inn_b, ib_s, ib_r, m, 2, True).wait_recv()
            res_b[m] = finish(inn_b, m)
            to_mate(m).start()

        @pl.when((i >= 2) & (i != pairs))
        def _():
            merge(block_at(i - 2))

    loads[15].wait()
    place = lax.broadcasted_iota(jnp.int32, (tokens, block), 1).astype(F32)

    def combine(m, rows):
        at = code_s[...] - (peer_of(m) * block).astype(F32)
        pick = jnp.where(place == at[:, 0:1], w_s[:, 0:1], 0.0) + jnp.where(
            place == at[:, 1:2], w_s[:, 1:2], 0.0
        )
        return dot(pick.astype(BF16), rows)

    mixed[...] = combine(0, merged[0])

    mix_copy(0).wait_recv()
    mix_copy(2).wait_recv()
    mixer_out[...] = (
        xp[tp].astype(F32) + from_sib[0].astype(F32) + from_far[...].astype(F32)
    ).astype(BF16)

    @pl.loop(0, pairs - 1)
    def _(i):
        m = block_at(i + 1)
        give_back(m).wait_recv()
        mixed[...] += combine(m, ret[m])

    expert_out[...] = mixed[...].astype(BF16)

    mix_copy(0).wait_send()
    mix_copy(2).wait_send()

    @pl.when((par == 1) & (pair < pairs - 1))
    def _():
        chain(0).wait_send()
        chain(1).wait_send()

    @pl.when(par == 0)
    def _():
        for copy in even_copies():
            copy.wait_send()

    for j in range(1, n_tp):
        dn_copy(j).wait_send()

    @pl.loop(0, pairs)
    def _(i):
        m = block_at(i)
        for hv in range(2):
            @pl.when(m >= NEAR)
            def _():
                trade_tok(m, 0, hv).wait_send()

            trade_tok(m, 1, hv).wait_send()
            trade_tok(m, 2, hv).wait_send()

        for kind in range(3):
            trade(inn_a, ia_s, ia_r, m, kind).wait_send()
            trade(inn_b, ib_s, ib_r, m, kind).wait_send()

        @pl.when(i < WHOLE)
        def _():
            cross(m).wait_send()
            cross_on(m).wait_send()

        @pl.when(i >= WHOLE)
        def _():
            cross_part(m).wait_send()
            for kind in range(3):
                share(m, kind).wait_send()

        to_mate(m).wait_send()

    @pl.loop(1, pairs)
    def _(m):
        for hv in range(2):
            dispatch(m, 0, hv).wait_send()

            @pl.when(m < NEAR)
            def _():
                dispatch(m, 1, hv).wait_send()

        give_back(m).wait_send()

    @pl.loop(1, n_ep)
    def _(m):
        count_copy(m).wait_send()


def body(
    queries, key_rows, value_rows, gate_rows, log_decay, head_gain, out_weight,
    expert_input, input_gain, route_ids, route_weight, expert_gate, expert_up, expert_down,
):
    n_tp = lax.axis_size("tp")
    n_ep = lax.axis_size("ep")
    width = out_weight.shape[1]
    tokens = expert_input.shape[0]
    n_experts = n_ep * expert_gate.shape[0]
    units = expert_gate.shape[2]
    capacity = 3 * tokens // n_experts
    block = 4 * capacity // 3
    chunk = block // n_tp
    pairs = n_ep // 2
    cols = width // n_tp
    length = queries.shape[0]
    heads = log_decay.shape[0]
    dk = queries.shape[1] // heads
    dv = value_rows.shape[1] // heads
    assert tokens == length and cols == heads * dv

    half = dk // 2
    frequency = theta_base ** (-np.arange(half) / half)
    frequency = np.concatenate([frequency, frequency])
    near = np.arange(length)[:, None] * frequency
    base = (np.arange(n_ep) * length)[:, None, None] * frequency
    tables = [jnp.asarray(f(a), F32) for a in (near, base) for f in (np.cos, np.sin)]

    wide = 512
    sizes = (n_ep, n_tp, heads, dk, dv)
    any_spec = pl.BlockSpec(memory_space=pl.ANY)
    vmem = pl.BlockSpec(memory_space=pltpu.VMEM)
    dma = pltpu.SemaphoreType.DMA
    V = pltpu.VMEM
    mixer_out, expert_out = pl.pallas_call(
        functools.partial(kernel, sizes),
        out_shape=(
            jax.ShapeDtypeStruct((length // n_tp, width), BF16),
            jax.ShapeDtypeStruct((tokens, cols), BF16),
        ),
        in_specs=[any_spec] * 18,
        out_specs=(vmem, vmem),
        scratch_shapes=[
            V((n_tp, tokens // n_tp, width), BF16),
            V((1, width), F32),
            V((tokens, 2), jnp.int32),
            V((tokens, 2), F32),
            V((tokens, 128), F32),
            V((pairs + NEAR, chunk, tokens), BF16),
            V((pairs + NEAR, chunk, width), BF16),
            V((pairs, block, width), BF16),
            V((pairs, capacity, width), BF16),
            V((width, 2 * units), BF16),
            V((n_tp, units, cols), BF16),
            V((pairs, n_tp, capacity, units), BF16),
            V((pairs, n_tp, capacity, units), BF16),
            V((pairs, capacity, cols), BF16),
            V((pairs, capacity, cols), BF16),
            V((pairs, capacity, cols), BF16),
            V((pairs, block, cols), BF16),
            V((pairs, block, cols), BF16),
            V((n_ep, 8, 128), F32),
            V((8, 128), F32),
            V((length, heads * dk), BF16),
            V((length, heads * dk), BF16),
            V((length, heads * dv), BF16),
            V((length, heads * dv), BF16),
            V((length, dk), F32),
            V((length, dk), F32),
            V((n_ep, 1, dk), F32),
            V((n_ep, 1, dk), F32),
            V((heads, length), F32),
            V((heads, length, 1), F32),
            V((heads, 1, length), F32),
            V((1, heads * dv), F32),
            V((2, heads * dv, wide), BF16),
            V((heads, length, dk), BF16),
            V((heads, length, dk), BF16),
            V((heads, length, dk), BF16),
            V((heads, length, dk), BF16),
            V((heads, dk, dv), F32),
            V((heads, dk, dv), BF16),
            V((heads, dk, dv), BF16),
            V((heads, dk, dv), BF16),
            V((heads, dk, dv), BF16),
            V((8, 128), F32),
            V((8, 128), F32),
            V((length, heads * dv), F32),
            V((length, heads * dv), BF16),
            V((2, length // n_tp, width), BF16),
            V((length // n_tp, width), BF16),
            dma((16,)),
            dma((2,)),
            dma((pairs, 2, 2)), dma((pairs, 2, 2)),
            dma((n_ep,)), dma((n_ep,)),
            dma((pairs, 3, 2)), dma((pairs, 3, 2)),
            dma((pairs,)), dma((pairs,)),
            dma((pairs, 3)), dma((pairs, 3)),
            dma((pairs, 3)), dma((pairs, 3)),
            dma((pairs, 3)), dma((pairs, 3)),
            dma((pairs,)), dma((pairs,)),
            dma((pairs,)), dma((pairs,)),
            dma((n_tp,)), dma((n_tp,)),
            dma((2,)), dma,
            dma((2,)), dma((2,)),
            dma((3,)), dma((3,)),
        ],
        compiler_params=pltpu.CompilerParams(
            collective_id=0, has_side_effects=True, vmem_limit_bytes=67_043_328
        ),
        name="fused",
    )(
        expert_input.reshape(n_tp, tokens // n_tp, width), input_gain[None, :],
        route_ids, route_weight, expert_gate, expert_up, expert_down,
        queries, key_rows, value_rows, gate_rows, tables[0], tables[1], tables[2], tables[3],
        log_decay, head_gain[None, :], out_weight,
    )
    return (mixer_out, expert_out)


def solution(mesh):
    placed = (
        P("ep", "tp"),
        P("ep", "tp"),
        P("ep", "tp"),
        P("ep", "tp"),
        P("tp", "ep"),
        P("tp"),
        P("tp", None),
        P("ep", None),
        P(),
        P("ep", None),
        P("ep", None),
        P("ep", None, "tp"),
        P("ep", None, "tp"),
        P("ep", "tp", None),
    )
    return jax.shard_map(
        body,
        mesh=mesh,
        in_specs=placed,
        out_specs=(P(("ep", "tp"), None), P("ep", "tp")),
        check_vma=False,
    )
```
